32 devices in a mesh: sp: 8 (over z, y), tp: 4 (over x, core).
Axes of the slice: x: 2, y: 2, z: 4, core: 2. Of those that a mesh axis runs over, the one named last changes fastest.
Arguments:
- residual: bfloat16 [1024, 2048], P(('sp', 'tp')), may hold values from -6 to 6
- query_content: bfloat16 [1024, 1024], P('sp', 'tp'), may hold values from -400 to 400
- query_rotary: bfloat16 [1024, 384], P('sp', 'tp'), may hold values from -16 to 16
- key_latent: bfloat16 [1024, 512], P('sp'), may hold values from -6 to 6
- rotary_key: bfloat16 [1024, 32], P('sp'), may hold values from -6 to 6
- latent_gain: float32 [512], replicated, may hold values from 0.1 to 1.9
- key_weight: bfloat16 [512, 1024], P(None, 'tp'), may hold values from -0.25 to 0.25
- value_weight: bfloat16 [512, 1024], P(None, 'tp'), may hold values from -0.25 to 0.25
- output_gain: float32 [1024], P('tp'), may hold values from 0.1 to 1.9
- output_weight: bfloat16 [1024, 2048], P('tp'), may hold values from -0.1875 to 0.1875
- mixer_gain: float32 [2048], replicated, may hold values from 0.1 to 1.9
- gate_weight: bfloat16 [2048, 5632], P('sp', 'tp'), may hold values from -0.125 to 0.125
- up_weight: bfloat16 [2048, 5632], P('sp', 'tp'), may hold values from -0.125 to 0.125
- down_weight: bfloat16 [5632, 2048], P('tp', 'sp'), may hold values from -0.078125 to 0.078125
Outputs:
- layer_out: bfloat16 [1024, 2048], P(('sp', 'tp'))
The draws below stay inside these ranges and needn't reach their ends.
All inputs are finite; a program needn't handle non-finite values.
Results may differ from the reference program's by a relative error of at most 0.015.
Values may be sent and summed in bfloat16 or wider, within the bound.
A program may use at most 128 MiB of HBM per device.

```python
import math
import jax
import jax.numpy as jnp
from jax import lax

D = 2048
FF = 5632
LATENT = 512
NARROW_HEADS = 8
WIDE_HEADS = 4
NARROW_DIM = 64
WIDE_DIM = 128
ROT_DIM = 32
TOKENS = 1024
CONTENT = 1024
ROTARY = 384
NARROW_DEV = 2
WIDE_DEV = 1
N_TP = 4


def draw_query_content(key, part):
    first_key = jax.random.fold_in(key, 0)
    width = NARROW_HEADS * NARROW_DIM + WIDE_HEADS * WIDE_DIM
    normal = jax.random.normal(first_key, (TOKENS, width), jnp.float32) * 2.5
    return jnp.clip(normal, -20.0, 20.0).astype(jnp.bfloat16)


def levels(stream_key, dims, shards, low, high):
    factor_of = 1.0
    for axis_at, blocks in shards:
        draws = jax.random.uniform(jax.random.fold_in(jax.random.fold_in(stream_key, 6), axis_at), (blocks,), jnp.float32, low / len(shards), high / len(shards))
        factor_of = factor_of * jnp.repeat(jnp.exp(draws), dims[axis_at] // blocks).reshape((-1,) + (1,) * (len(dims) - 1 - axis_at))
    return factor_of


def gaussian(rng, shape, deviation, most, pieces=(), kind=jnp.bfloat16):
    values = deviation * jax.random.normal(rng, shape, jnp.float32)
    if pieces:
        values = values * levels(rng, shape, pieces, -0.22, 0.18)
    return jnp.clip(values, -most, most).astype(kind)


def setup_inputs(seed: int = 0) -> dict:
    streams_of = jax.random.split(jax.random.key(seed), 15)
    residual = gaussian(streams_of[0], (TOKENS, D), 1.0, 6.0, ((0, 32),))
    query_content = draw_query_content(jax.random.fold_in(streams_of[14], 71), 0)
    query_rotary = gaussian(streams_of[2], (TOKENS, ROTARY), 2.5, 16.0, ((0, 8), (1, 4)))
    key_latent = gaussian(streams_of[3], (TOKENS, LATENT), 1.0, 6.0, ((0, 8),))
    rotary_key = gaussian(streams_of[4], (TOKENS, ROT_DIM), 1.0, 6.0, ((0, 8),))
    latent_gain = jnp.clip(1.0 + 0.18 * jax.random.normal(streams_of[5], (LATENT,), jnp.float32), 0.1, 1.9)
    key_weight = gaussian(streams_of[6], (LATENT, CONTENT), LATENT ** -0.5, 0.25, ((1, 4),))
    value_weight = gaussian(streams_of[7], (LATENT, CONTENT), LATENT ** -0.5, 0.25, ((1, 4),))
    output_gain = jnp.clip(1.0 + 0.18 * jax.random.normal(streams_of[8], (CONTENT,), jnp.float32), 0.1, 1.9)
    output_weight = gaussian(streams_of[9], (CONTENT, D), CONTENT ** -0.5, 0.1875, ((0, 4),))
    mixer_gain = jnp.clip(1.0 + 0.18 * jax.random.normal(streams_of[10], (D,), jnp.float32), 0.1, 1.9)
    gate_weight = gaussian(streams_of[11], (D, FF), D ** -0.5, 0.125, ((0, 8), (1, 4)))
    up_weight = gaussian(streams_of[12], (D, FF), D ** -0.5, 0.125, ((0, 8), (1, 4)))
    down_weight = gaussian(streams_of[13], (FF, D), FF ** -0.5, 0.078125, ((0, 4), (1, 8)))
    return {"residual": residual, "query_content": query_content, "query_rotary": query_rotary, "key_latent": key_latent, "rotary_key": rotary_key, "latent_gain": latent_gain, "key_weight": key_weight, "value_weight": value_weight, "output_gain": output_gain, "output_weight": output_weight, "mixer_gain": mixer_gain, "gate_weight": gate_weight, "up_weight": up_weight, "down_weight": down_weight}


epsilon = 1e-06
rope_base = 500000.0

def stored(values):
    return lax.optimization_barrier(values.astype(jnp.bfloat16))

def normalize(values):
    values = values.astype(jnp.float32)
    return values * lax.rsqrt(lax.optimization_barrier(jnp.mean(values * values, axis=-1, keepdims=True)) + epsilon)

def rotate(values, positions):
    half_width = values.shape[-1] // 2
    inverse = 1.0 / jnp.power(rope_base, jnp.arange(0, 2 * half_width, 2, dtype=jnp.float32) / (2 * half_width))
    angles = positions.astype(jnp.float32)[:, None] * inverse[None, :]
    table_shape = (angles.shape[0],) + (1,) * (values.ndim - 2) + (half_width,)
    cosine_table = jnp.cos(angles).reshape(table_shape)
    sine_table = jnp.sin(angles).reshape(table_shape)
    first_half = values[..., :half_width]
    second_half = values[..., half_width:]
    return jnp.concatenate([first_half * cosine_table - second_half * sine_table, second_half * cosine_table + first_half * sine_table], axis=-1)

def split_groups(whole, narrow_size, wide_size):
    row_count = whole.shape[0]
    blocks = whole.reshape(row_count, N_TP, -1)
    narrow_cols = NARROW_DEV * narrow_size
    narrow = blocks[:, :, :narrow_cols].reshape(row_count, N_TP * NARROW_DEV, narrow_size)
    wide = blocks[:, :, narrow_cols:].reshape(row_count, N_TP * WIDE_DEV, wide_size)
    return (narrow, wide)

def join_groups(narrow, wide):
    row_count = narrow.shape[0]
    return jnp.concatenate([narrow.reshape(row_count, N_TP, -1), wide.reshape(row_count, N_TP, -1)], axis=2).reshape(row_count, -1)

def attend(query_part, rotary_part, key_part, rotary_keys, value_part, factor):
    key_float = key_part.astype(jnp.float32)
    rotary_float = rotary_keys.astype(jnp.float32)
    value_float = value_part.astype(jnp.float32)
    row_count = query_part.shape[0]
    block_rows = math.gcd(512, row_count)

    def one_block(offset):
        query_block = lax.dynamic_slice_in_dim(query_part, offset, block_rows, 0).astype(jnp.float32)
        rotary_block = lax.dynamic_slice_in_dim(rotary_part, offset, block_rows, 0).astype(jnp.float32)
        scores = (jnp.einsum('qhd,khd->hqk', query_block, key_float) + jnp.einsum('qhd,kd->hqk', rotary_block, rotary_float)) * factor
        largest = lax.optimization_barrier(jnp.max(scores, axis=-1, keepdims=True))
        powers = jnp.exp(scores - largest)
        totals = lax.optimization_barrier(jnp.sum(powers, axis=-1))
        weights = stored(powers).astype(jnp.float32)
        summed = jnp.einsum('hqk,khd->qhd', weights, value_float)
        return summed / jnp.transpose(totals)[:, :, None]
    offsets = jnp.arange(0, row_count, block_rows, dtype=jnp.int32)
    result = lax.map(one_block, offsets)
    return result.reshape(row_count, result.shape[2], result.shape[3])

def reference(residual, query_content, query_rotary, key_latent, rotary_key, latent_gain, key_weight, value_weight, output_gain, output_weight, mixer_gain, gate_weight, up_weight, down_weight):
    row_count = key_latent.shape[0]
    positions = jnp.arange(row_count, dtype=jnp.int32)
    latent = stored(normalize(key_latent) * latent_gain.astype(jnp.float32))
    key_content = stored(jnp.dot(latent, key_weight, preferred_element_type=jnp.float32))
    value_rows = stored(jnp.dot(latent, value_weight, preferred_element_type=jnp.float32))
    rot_keys = stored(rotate(rotary_key.astype(jnp.float32), positions))
    turned = rotate(query_rotary.astype(jnp.float32).reshape(row_count, -1, ROT_DIM), positions)
    rot_queries = stored(turned).reshape(row_count, -1)
    query_narrow, query_wide = split_groups(query_content, NARROW_DIM, WIDE_DIM)
    rotary_narrow, rotary_wide = split_groups(rot_queries, ROT_DIM, ROT_DIM)
    key_narrow, key_wide = split_groups(key_content, NARROW_DIM, WIDE_DIM)
    value_narrow, value_wide = split_groups(value_rows, NARROW_DIM, WIDE_DIM)
    out_narrow = attend(query_narrow, rotary_narrow, key_narrow, rot_keys, value_narrow, (NARROW_DIM + ROT_DIM) ** (-0.5))
    out_wide = attend(query_wide, rotary_wide, key_wide, rot_keys, value_wide, (WIDE_DIM + ROT_DIM) ** (-0.5))
    mixed = stored(join_groups(normalize(out_narrow), normalize(out_wide)) * output_gain.astype(jnp.float32))
    projected = jnp.dot(mixed, output_weight, preferred_element_type=jnp.float32)
    middle = stored(residual.astype(jnp.float32) + projected)
    normed = stored(normalize(middle) * mixer_gain.astype(jnp.float32))
    gate_sums = jnp.dot(normed, gate_weight, preferred_element_type=jnp.float32)
    up_sums = jnp.dot(normed, up_weight, preferred_element_type=jnp.float32)
    hidden = stored(jax.nn.silu(gate_sums) * up_sums)
    block_width = FF // N_TP
    channel_out = jnp.zeros((row_count, D), jnp.float32)
    for block_index in range(N_TP):
        columns = hidden[:, block_index * block_width:(block_index + 1) * block_width]
        weight_rows = down_weight[block_index * block_width:(block_index + 1) * block_width]
        channel_out = channel_out + stored(jnp.dot(columns, weight_rows, preferred_element_type=jnp.float32)).astype(jnp.float32)
    return (middle.astype(jnp.float32) + channel_out).astype(jnp.bfloat16)
```

```python
import functools

import jax
import jax.numpy as jnp
import numpy as np
from jax import lax
from jax.experimental import pallas as pl
from jax.experimental.pallas import tpu as pltpu
from jax.sharding import PartitionSpec as P

NARROW_HEADS = 8
WIDE_HEADS = 4
NARROW_DIM = 64
WIDE_DIM = 128
ROT_DIM = 32


epsilon = 1e-06
rope_base = 500000.0


def normalize(values):
    values = values.astype(jnp.float32)
    return values * lax.rsqrt(jnp.mean(values * values, axis=-1, keepdims=True) + epsilon)


def rotate(values, positions):
    half_width = values.shape[-1] // 2
    inverse = 1.0 / jnp.power(
        rope_base, jnp.arange(0, 2 * half_width, 2, dtype=jnp.float32) / (2 * half_width)
    )
    angles = positions.astype(jnp.float32)[:, None] * inverse[None, :]
    table_shape = (angles.shape[0],) + (1,) * (values.ndim - 2) + (half_width,)
    cosine_table = jnp.cos(angles).reshape(table_shape)
    sine_table = jnp.sin(angles).reshape(table_shape)
    first_half = values[..., :half_width]
    second_half = values[..., half_width:]
    return jnp.concatenate(
        [
            first_half * cosine_table - second_half * sine_table,
            second_half * cosine_table + first_half * sine_table,
        ],
        axis=-1,
    )


def group_update(carried, query_part, rotary_part, key_part, rotary_keys, value_part, factor):
    running_max, totals, accumulated = carried
    scores = (
        jnp.einsum("qhd,khd->hqk", query_part, key_part, preferred_element_type=jnp.float32)
        + jnp.einsum("qhd,kd->hqk", rotary_part, rotary_keys, preferred_element_type=jnp.float32)
    ) * factor
    new_max = jnp.max(scores, axis=-1)
    shrink = jnp.exp(running_max - new_max)
    powers = jnp.exp(scores - new_max[..., None])
    totals = totals * shrink + jnp.sum(powers, axis=-1)
    added = jnp.einsum(
        "hqk,khd->qhd", powers.astype(jnp.bfloat16), value_part, preferred_element_type=jnp.float32
    )
    accumulated = accumulated * jnp.transpose(shrink)[:, :, None] + added
    return (new_max, totals, accumulated)


def on_device(
    residual,
    query_content,
    query_rotary,
    key_latent,
    rotary_key,
    latent_gain,
    key_weight,
    value_weight,
    output_gain,
    output_weight,
    mixer_gain,
    gate_weight,
    up_weight,
    down_weight,
):
    tp_count = lax.axis_size("tp")
    narrow_dev = NARROW_HEADS // tp_count
    wide_dev = WIDE_HEADS // tp_count
    row_count = key_latent.shape[0]
    positions = lax.axis_index("sp") * row_count + lax.iota(jnp.int32, row_count)
    latent = (normalize(key_latent) * latent_gain).astype(jnp.bfloat16)
    key_rows = jnp.dot(latent, key_weight, preferred_element_type=jnp.float32).astype(jnp.bfloat16)
    value_rows = jnp.dot(latent, value_weight, preferred_element_type=jnp.float32).astype(
        jnp.bfloat16
    )
    rot_keys = rotate(rotary_key.astype(jnp.float32), positions).astype(jnp.bfloat16)
    head_count = narrow_dev + wide_dev
    rot_queries = rotate(
        query_rotary.astype(jnp.float32).reshape(row_count, head_count, ROT_DIM), positions
    ).astype(jnp.bfloat16)
    narrow_cols = narrow_dev * NARROW_DIM
    query_narrow = query_content[:, :narrow_cols].reshape(row_count, narrow_dev, NARROW_DIM)
    query_wide = query_content[:, narrow_cols:].reshape(row_count, wide_dev, WIDE_DIM)
    rotary_narrow = rot_queries[:, :narrow_dev]
    rotary_wide = rot_queries[:, narrow_dev:]
    narrow_factor = (NARROW_DIM + ROT_DIM) ** (-0.5)
    wide_factor = (WIDE_DIM + ROT_DIM) ** (-0.5)

    def start_state(count, width):
        return (
            jnp.full((count, row_count), -jnp.inf, jnp.float32),
            jnp.zeros((count, row_count), jnp.float32),
            jnp.zeros((row_count, count, width), jnp.float32),
        )

    carried = (start_state(narrow_dev, NARROW_DIM), start_state(wide_dev, WIDE_DIM))
    piece_keys = lax.all_gather(key_rows, "sp", axis=0, tiled=True)
    piece_rotary = lax.all_gather(rot_keys, "sp", axis=0, tiled=True)
    piece_values = lax.all_gather(value_rows, "sp", axis=0, tiled=True)
    length = piece_keys.shape[0]
    narrow_keys = piece_keys[:, :narrow_cols].reshape(length, narrow_dev, NARROW_DIM)
    wide_keys = piece_keys[:, narrow_cols:].reshape(length, wide_dev, WIDE_DIM)
    narrow_values = piece_values[:, :narrow_cols].reshape(length, narrow_dev, NARROW_DIM)
    wide_values = piece_values[:, narrow_cols:].reshape(length, wide_dev, WIDE_DIM)
    narrow_state = group_update(
        carried[0],
        query_narrow,
        rotary_narrow,
        narrow_keys,
        piece_rotary,
        narrow_values,
        narrow_factor,
    )
    wide_state = group_update(
        carried[1], query_wide, rotary_wide, wide_keys, piece_rotary, wide_values, wide_factor
    )
    narrow_state, wide_state = (narrow_state, wide_state)

    def finish(carried):
        return normalize(carried[2] / jnp.transpose(carried[1])[:, :, None]).reshape(row_count, -1)

    mixed = (
        jnp.concatenate([finish(narrow_state), finish(wide_state)], axis=1) * output_gain
    ).astype(jnp.bfloat16)
    whole_output = lax.all_gather(output_weight, "tp", axis=0, tiled=True)
    regrouped = lax.all_to_all(mixed, "tp", split_axis=0, concat_axis=1, tiled=True)
    projected = jnp.dot(regrouped, whole_output, preferred_element_type=jnp.float32)
    middle = (residual.astype(jnp.float32) + projected).astype(jnp.bfloat16)
    normed = (normalize(middle) * mixer_gain).astype(jnp.bfloat16)
    block_normed = lax.all_gather(normed, "tp", axis=0, tiled=True)
    gate_sums = jnp.dot(
        block_normed,
        lax.all_gather(gate_weight, "sp", axis=0, tiled=True),
        preferred_element_type=jnp.float32,
    )
    up_sums = jnp.dot(
        block_normed,
        lax.all_gather(up_weight, "sp", axis=0, tiled=True),
        preferred_element_type=jnp.float32,
    )
    down_whole = lax.all_gather(down_weight, "sp", axis=1, tiled=True)
    hidden = (jax.nn.silu(gate_sums) * up_sums).astype(jnp.bfloat16)
    channel_out = lax.psum_scatter(
        jnp.dot(hidden, down_whole, preferred_element_type=jnp.float32).astype(jnp.bfloat16),
        "tp",
        scatter_dimension=0,
        tiled=True,
    ).astype(jnp.float32)
    return (middle.astype(jnp.float32) + channel_out).astype(jnp.bfloat16)


MESH = pl.DeviceIdType.MESH
LANES = 128
PAIR = 2


def kernel(
    n_sp,
    query_hbm,
    latent_hbm,
    latent_gain_ref,
    key_weight_hbm,
    value_weight_hbm,
    output_gain_ref,
    mixer_gain_ref,
    cos_hbm,
    sin_hbm,
    residual_hbm,
    output_weight_hbm,
    turn_hbm,
    rotary_hbm,
    gate_ref,
    up_ref,
    down_ref,
    out_ref,
    query_ref,
    latent_ref,
    key_weight_ref,
    value_weight_ref,
    cos_ref,
    sin_ref,
    residual_ref,
    output_weight_ref,
    turn_ref,
    rotary_ref,
    lat_all,
    rot_all,
    rot_keys,
    keys,
    values,
    projected,
    to_core_rows,
    from_core_rows,
    to_x_rows,
    from_x_rows,
    middle,
    normed,
    gate_all,
    up_all,
    down_all,
    gates,
    hidden,
    part,
    from_core,
    to_x,
    from_x,
    to_z,
    from_z,
    summed_up,
    send_sems,
    recv_sems,
    local_sems,
):
    n_z = n_sp // PAIR
    s = lax.axis_index("sp")
    t = lax.axis_index("tp")
    z, y = s // PAIR, lax.rem(s, PAIR)
    x, c = t // PAIR, lax.rem(t, PAIR)
    rows, depth = latent_ref.shape
    half = rows // PAIR
    sibling = (s, x * PAIR + 1 - c)
    across = (s, (1 - x) * PAIR + c)
    beside = (z * PAIR + 1 - y, t)
    f32 = jnp.float32
    bf16 = jnp.bfloat16

    def other(step):
        if step == 0:
            return z
        if step == 1:
            return z + 1 - 2 * lax.rem(z, PAIR)
        if step == 2:
            return lax.rem(z + PAIR, n_z)
        return n_z - 1 - z

    def z_id(step):
        return (other(step) * PAIR + y, t)

    barrier = pltpu.get_barrier_semaphore()
    greeted = [z_id(k) for k in range(1, n_z)] + [beside, sibling, across]
    for device in greeted:
        pl.semaphore_signal(barrier, inc=1, device_id=device, device_id_type=MESH)

    used = [0]
    locals_used = [0]
    sent = []

    def local(src, dst, go=None):
        copy = pltpu.make_async_copy(src, dst, local_sems.at[locals_used[0]])
        locals_used[0] += 1
        if go is None:
            copy.start()
        else:
            pl.when(go)(copy.start)
        return (copy, go)

    def landed(pair):
        copy, go = pair
        if go is None:
            copy.wait()
        else:
            pl.when(go)(copy.wait)

    def send(src, dst, device, go=None, comes=None):
        copy = pltpu.make_async_remote_copy(
            src_ref=src,
            dst_ref=dst,
            send_sem=send_sems.at[used[0]],
            recv_sem=recv_sems.at[used[0]],
            device_id=device,
            device_id_type=MESH,
        )
        used[0] += 1
        if go is None:
            copy.start()
        else:
            pl.when(go)(copy.start)
        sent.append((copy, go))
        return (copy, comes)

    def arrived(*pairs):
        for copy, comes in pairs:
            if comes is None:
                copy.wait_recv()
            else:
                pl.when(comes)(copy.wait_recv)

    locals_first = [
        local(latent_hbm, latent_ref),
        local(rotary_hbm, rotary_ref),
        local(turn_hbm, turn_ref),
        local(query_hbm, query_ref),
        local(key_weight_hbm, key_weight_ref),
        local(value_weight_hbm, value_weight_ref),
        local(cos_hbm, cos_ref),
        local(sin_hbm, sin_ref),
    ]
    locals_rest = [
        local(output_weight_hbm, output_weight_ref),
        local(residual_hbm, residual_ref),
    ]

    width = gate_all.shape[1]
    total_width = gate_ref.shape[1]
    slab = gate_ref.shape[0]
    main = width - LANES
    short = n_z * width - total_width

    def full(owner):
        return jnp.where(c == 0, owner, n_z - 1 - owner) > 0

    def first(owner):
        return pl.multiple_of(jnp.maximum(owner * width - (1 - c) * short, 0), LANES)

    def span(owner):
        return pl.ds(pl.multiple_of(owner * slab, slab), slab)

    mine = span(s)
    mine_full = full(z)
    low, high = pl.ds(0, main), pl.ds(main, LANES)
    down_cols = pl.ds(pl.multiple_of(y * slab, slab), slab)

    def unit_parts(owner):
        start = first(owner)
        last = jnp.minimum(start + main, total_width - LANES)
        return pl.ds(start, main), pl.ds(pl.multiple_of(last, LANES), LANES)

    def wide_ends(ref, buffer, owner):
        a, b = unit_parts(owner)
        return [
            (ref.at[:, a], buffer.at[mine, low]),
            (ref.at[:, b], buffer.at[mine, high]),
        ]

    def down_ends(owner, step):
        a, b = unit_parts(owner)
        return [
            (down_ref.at[a], down_all.at[step, low, down_cols]),
            (down_ref.at[b], down_all.at[step, high, down_cols]),
        ]

    def send_parts(ends, device, go):
        return [
            send(*ends[0], device),
            send(*ends[1], device, go=go, comes=mine_full),
        ]

    def local_parts(ends):
        return [local(*ends[0]), local(*ends[1], go=mine_full)]

    def gate_to(k):
        return send_parts(wide_ends(gate_ref, gate_all, other(k)), z_id(k), full(other(k)))

    def up_to(k):
        return send_parts(wide_ends(up_ref, up_all, other(k)), z_id(k), full(other(k)))

    def down_to(k):
        return send_parts(down_ends(other(k), k), z_id(k), full(other(k)))

    def relay_wide(copies, buffer, step):
        arrived(*copies)
        block = span(other(step) * PAIR + y)
        ends = [(buffer.at[block, cols],) * 2 for cols in (low, high)]
        return send_parts(ends, beside, mine_full)

    def relay_down(copies, step):
        arrived(*copies)
        ends = [(down_all.at[step, units, down_cols],) * 2 for units in (low, high)]
        return send_parts(ends, beside, mine_full)

    weights_here = (
        local_parts(wide_ends(gate_ref, gate_all, z))
        + local_parts(wide_ends(up_ref, up_all, z))
        + local_parts(down_ends(z, 0))
    )

    @pl.when(jnp.logical_not(mine_full))
    def _():
        down_all[:, main:, :] = jnp.zeros((n_z, LANES, down_all.shape[2]), bf16)

    for copy in locals_first[:2]:
        landed(copy)
    pl.semaphore_wait(barrier, len(greeted))

    half_rows = pl.ds(pl.multiple_of(c * half, half), half)
    rot_half = rotary_ref.shape[0] // PAIR
    rot_rows = pl.ds(pl.multiple_of(c * rot_half, rot_half), rot_half)

    def token_half(owner):
        return pl.ds(pl.multiple_of(owner * rows + c * half, half), half)

    def send_latent(device):
        return [
            send(latent_ref.at[half_rows], lat_all.at[token_half(s)], device),
            send(rotary_ref.at[rot_rows], rot_all.at[s, rot_rows], device),
        ]

    def pass_latent(owner, device):
        place = token_half(owner)
        return [
            send(lat_all.at[place], lat_all.at[place], device),
            send(rot_all.at[owner, rot_rows], rot_all.at[owner, rot_rows], device),
        ]

    steps = list(range(1, n_z))
    far_first = [2, 3, 1]
    latent_z = {k: send_latent(z_id(k)) for k in far_first}
    latent_y = {0: send_latent(beside)}
    gate_z = {k: gate_to(k) for k in far_first}
    up_z = {2: up_to(2)}
    gate_y = [
        send_parts(wide_ends(gate_ref, gate_all, z), beside, mine_full),
    ]

    latent_core = []
    for k in (1, 2, 3):
        arrived(*latent_z[k])
        owner = other(k) * PAIR + y
        latent_y[k] = pass_latent(owner, beside)
        latent_core += pass_latent(owner, sibling)
    up_y = [send_parts(wide_ends(up_ref, up_all, z), beside, mine_full)]
    down_y = {0: send_parts(down_ends(z, 0), beside, mine_full)}
    for k in (0, 1, 2, 3):
        arrived(*latent_y[k])
        latent_core += pass_latent(other(k) * PAIR + 1 - y, sibling)
    for copy in locals_first[2:]:
        landed(copy)

    gain = latent_gain_ref[...]
    here = pl.ds(pl.multiple_of(s * rows, rows), rows)
    lat_all[here, :] = latent_ref[...]
    rot_all[s] = rotary_ref[...]
    arrived(*latent_core)

    def project(block, _):
        place = pl.ds(pl.multiple_of(block * rows, rows), rows)
        raw = lat_all[place, :].astype(f32)
        scale = lax.rsqrt(jnp.mean(raw * raw, axis=-1, keepdims=True) + epsilon)
        latent = (raw * scale * gain).astype(bf16)
        keys[place, :] = jnp.dot(latent, key_weight_ref[...], preferred_element_type=f32).astype(
            bf16
        )
        values[place, :] = jnp.dot(
            latent, value_weight_ref[...], preferred_element_type=f32
        ).astype(bf16)
        return 0

    lax.fori_loop(0, n_sp, project, 0)

    def turn(raw, cosine, sine):
        top, bottom = raw[:rot_half].astype(f32), raw[rot_half:].astype(f32)
        return jnp.concatenate(
            [top * cosine - bottom * sine, bottom * cosine + top * sine], axis=0
        )

    for block in range(n_sp):
        cols = slice(block * rows, (block + 1) * rows)
        rot_keys[:, cols] = turn(rot_all[block], cos_ref[block], sin_ref[block]).astype(bf16)

    content = query_ref.shape[1]
    rot_width = rotary_ref.shape[0]
    head_count = turn_ref.shape[0] // rot_width
    my_cos, my_sin = cos_ref[s], sin_ref[s]
    turned = [
        turn(turn_ref[index * rot_width : (index + 1) * rot_width], my_cos, my_sin)
        for index in range(head_count)
    ]
    turned.append(jnp.zeros((LANES - head_count * rot_width, rows), f32))
    turned = jnp.transpose(jnp.concatenate(turned, axis=0)).astype(bf16)

    wide_dev = (content - head_count * NARROW_DIM) // (WIDE_DIM - NARROW_DIM)
    sizes = [NARROW_DIM] * (head_count - wide_dev) + [WIDE_DIM] * wide_dev
    contract = (((1,), (1,)), ((), ()))
    heads = []
    start = 0
    for index, size in enumerate(sizes):
        cols = slice(start, start + size)
        scores = lax.dot_general(
            query_ref[:, cols], keys[:, cols], contract, preferred_element_type=f32
        )
        scores = scores + jnp.dot(
            turned[:, index * rot_width : (index + 1) * rot_width],
            rot_keys[...],
            preferred_element_type=f32,
        )
        scores = scores * (size + ROT_DIM) ** (-0.5)
        powers = jnp.exp(scores - jnp.max(scores, axis=-1, keepdims=True))
        totals = jnp.sum(powers, axis=-1, keepdims=True)
        summed = jnp.dot(powers.astype(bf16), values[:, cols], preferred_element_type=f32)
        attended = summed / totals
        scale = lax.rsqrt(jnp.mean(attended * attended, axis=-1, keepdims=True) + epsilon)
        heads.append(attended * scale)
        start += size
    mixed = (jnp.concatenate(heads, axis=1) * output_gain_ref[...]).astype(bf16)

    for copy in locals_rest:
        landed(copy)
    projected[...] = jnp.dot(
        mixed, output_weight_ref[...], preferred_element_type=f32
    ).reshape(projected.shape)
    to_core_rows[...] = projected[:, 1 - c].astype(bf16)
    rows_core = send(to_core_rows, from_core_rows, sibling)
    gate_y.append(relay_wide(gate_z[1], gate_all, 1))
    arrived(rows_core)
    to_x_rows[...] = (projected[1 - x, c] + from_core_rows[1 - x].astype(f32)).astype(bf16)
    rows_x = send(to_x_rows, from_x_rows, across)
    near_rows = projected[x, c] + from_core_rows[x].astype(f32) + residual_ref[...].astype(f32)
    gate_y.append(relay_wide(gate_z[2], gate_all, 2))
    arrived(rows_x)
    middle[...] = (near_rows + from_x_rows[...].astype(f32)).astype(bf16)
    tall = middle[...].astype(f32)
    scale = lax.rsqrt(jnp.mean(tall * tall, axis=-1, keepdims=True) + epsilon)
    normed[z, t] = (tall * scale * mixer_gain_ref[...]).astype(bf16)

    def pass_normed(owner, place, device):
        return send(normed.at[owner, place], normed.at[owner, place], device)

    normed_z = {k: pass_normed(z, t, z_id(k)) for k in far_first}
    normed_x = {0: pass_normed(z, t, across)}
    normed_core = [pass_normed(z, t, sibling)]
    for k in (3, 1):
        up_z[k] = up_to(k)
    down_z = {k: down_to(k) for k in (1, 2, 3)}
    gate_y.append(relay_wide(gate_z[3], gate_all, 3))
    up_y.append(relay_wide(up_z[2], up_all, 2))

    for k in (1, 2, 3):
        arrived(normed_z[k])
        normed_x[k] = pass_normed(other(k), t, across)
        normed_core.append(pass_normed(other(k), t, sibling))
    far_t = (1 - x) * PAIR + c
    for k in range(n_z):
        arrived(normed_x[k])
        normed_core.append(pass_normed(other(k), far_t, sibling))
    for copy in weights_here:
        landed(copy)
    for copies in gate_y:
        arrived(*copies)
    arrived(*normed_core)

    d_model = middle.shape[1]

    def gate_units(block, _):
        place = pl.ds(pl.multiple_of(block * rows, rows), rows)
        left = normed[block].reshape(rows, d_model)
        gates[place, :] = jnp.dot(left, gate_all[...], preferred_element_type=f32)
        return 0

    lax.fori_loop(0, n_z, gate_units, 0)

    for k in (3, 1):
        up_y.append(relay_wide(up_z[k], up_all, k))
    for copies in up_y:
        arrived(*copies)

    lane = lax.broadcasted_iota(jnp.int32, (rows, width), 1)
    fresh = lane < jnp.where(mine_full, width, main)

    def units(block, _):
        place = pl.ds(pl.multiple_of(block * rows, rows), rows)
        left = normed[block].reshape(rows, d_model)
        ups = jnp.dot(left, up_all[...], preferred_element_type=f32)
        gate = gates[place, :]
        value = gate / (1.0 + jnp.exp(-gate)) * ups
        hidden[place, :] = jnp.where(fresh, value, 0.0).astype(bf16)
        return 0

    lax.fori_loop(0, n_z, units, 0)

    down_y[1] = relay_down(down_z[1], 1)
    core_copies, x_copies, z_copies = [], [], []
    for step in range(n_z + 2):
        n = step - 2
        if 0 <= n < n_z:
            arrived(x_copies[n])
            to_z[n] = (to_x[n, :, x].astype(f32) + from_x[n].astype(f32)).astype(bf16)
            z_copies.append(
                {
                    k: send(to_z.at[n, other(k)], from_z.at[n, k - 1], z_id(k))
                    for k in far_first
                }
            )
        n = step - 1
        if 0 <= n < n_z:
            arrived(core_copies[n])
            to_x[n] = (part[n, :, :, c].astype(f32) + from_core[n].astype(f32)).astype(bf16)
            x_copies.append(send(to_x.at[n, :, 1 - x], from_x.at[n], across))
        n = step
        if n < n_z:
            if 2 <= n + 1 < n_z:
                down_y[n + 1] = relay_down(down_z[n + 1], n + 1)
            arrived(*down_y[n])
            product = jnp.dot(hidden[...], down_all[n], preferred_element_type=f32)
            part[n] = product.astype(bf16).reshape(part.shape[1:])
            core_copies.append(send(part.at[n, :, :, 1 - c], from_core.at[n], sibling))
    chunk = part.shape[-1]

    def cols_of(step):
        return pl.ds(pl.multiple_of(other(step) * chunk, chunk), chunk)

    for n in range(n_z):
        cols = cols_of(n)
        summed_up[:, cols] = middle[:, cols].astype(f32) + to_z[n, z].astype(f32)
    for n in range(n_z):
        for k in steps:
            arrived(z_copies[n][k])
            cols = cols_of(n ^ k)
            summed_up[:, cols] = summed_up[:, cols] + from_z[n, k - 1].astype(f32)
    out_ref[...] = summed_up[...].astype(bf16)
    for copy, go in sent:
        if go is None:
            copy.wait_send()
        else:
            pl.when(go)(copy.wait_send)


def fused(
    n_sp,
    residual,
    query_content,
    query_rotary,
    key_latent,
    rotary_key,
    latent_gain,
    key_weight,
    value_weight,
    output_gain,
    output_weight,
    mixer_gain,
    gate_weight,
    up_weight,
    down_weight,
):
    n_z = n_sp // PAIR
    rows, latent_width = key_latent.shape
    strip, d_model = residual.shape
    tokens = rows * n_sp
    content = query_content.shape[1]
    turn_width = query_rotary.shape[1]
    half_width = ROT_DIM // 2
    inverse = np.float32(1.0) / np.power(
        np.float32(rope_base), np.arange(0, ROT_DIM, 2, dtype=np.float32) / np.float32(ROT_DIM)
    )
    angles = np.arange(tokens, dtype=np.float32)[:, None] * inverse[None, :].astype(np.float32)
    angles = angles.reshape(n_sp, rows, half_width).transpose(0, 2, 1)
    cos_table = np.cos(angles).astype(np.float32)
    sin_table = np.sin(angles).astype(np.float32)
    tiles = gate_weight.shape[1] // LANES
    width = -(-tiles // n_z) * LANES
    slab = rows * n_z
    chunk = d_model // n_z
    bf16 = jnp.bfloat16
    n_copies = 16 * n_sp
    vmem = pl.BlockSpec(memory_space=pltpu.VMEM)
    anywhere = pl.BlockSpec(memory_space=pl.ANY)
    return pl.pallas_call(
        functools.partial(kernel, n_sp),
        out_shape=jax.ShapeDtypeStruct((strip, d_model), bf16),
        in_specs=[anywhere] * 2 + [vmem] + [anywhere] * 2 + [vmem] * 2 + [anywhere] * 9,
        out_specs=vmem,
        scratch_shapes=[
            pltpu.VMEM((rows, content), bf16),
            pltpu.VMEM((rows, latent_width), bf16),
            pltpu.VMEM((latent_width, content), bf16),
            pltpu.VMEM((latent_width, content), bf16),
            pltpu.VMEM((n_sp, half_width, rows), jnp.float32),
            pltpu.VMEM((n_sp, half_width, rows), jnp.float32),
            pltpu.VMEM((strip, d_model), bf16),
            pltpu.VMEM((content, d_model), bf16),
            pltpu.VMEM((turn_width, rows), bf16),
            pltpu.VMEM((ROT_DIM, rows), bf16),
            pltpu.VMEM((tokens, latent_width), bf16),
            pltpu.VMEM((n_sp, ROT_DIM, rows), bf16),
            pltpu.VMEM((ROT_DIM, tokens), bf16),
            pltpu.VMEM((tokens, content), bf16),
            pltpu.VMEM((tokens, content), bf16),
            pltpu.VMEM((PAIR, PAIR, strip, d_model), jnp.float32),
            pltpu.VMEM((PAIR, strip, d_model), bf16),
            pltpu.VMEM((PAIR, strip, d_model), bf16),
            pltpu.VMEM((strip, d_model), bf16),
            pltpu.VMEM((strip, d_model), bf16),
            pltpu.VMEM((strip, d_model), bf16),
            pltpu.VMEM((n_z, PAIR * PAIR, strip, d_model), bf16),
            pltpu.VMEM((d_model, width), bf16),
            pltpu.VMEM((d_model, width), bf16),
            pltpu.VMEM((n_z, width, chunk), bf16),
            pltpu.VMEM((slab, width), jnp.float32),
            pltpu.VMEM((slab, width), bf16),
            pltpu.VMEM((n_z, n_z, PAIR, PAIR, strip, chunk), bf16),
            pltpu.VMEM((n_z, n_z, PAIR, strip, chunk), bf16),
            pltpu.VMEM((n_z, n_z, PAIR, strip, chunk), bf16),
            pltpu.VMEM((n_z, n_z, strip, chunk), bf16),
            pltpu.VMEM((n_z, n_z, strip, chunk), bf16),
            pltpu.VMEM((n_z, n_z - 1, strip, chunk), bf16),
            pltpu.VMEM((strip, d_model), jnp.float32),
            pltpu.SemaphoreType.DMA((n_copies,)),
            pltpu.SemaphoreType.DMA((n_copies,)),
            pltpu.SemaphoreType.DMA((2 * n_sp,)),
        ],
        compiler_params=pltpu.CompilerParams(
            collective_id=0, has_side_effects=True, vmem_limit_bytes=60 * 1024 * 1024
        ),
        name="layer",
    )(
        query_content,
        key_latent,
        latent_gain.reshape(1, -1),
        key_weight,
        value_weight,
        output_gain.reshape(1, -1),
        mixer_gain.reshape(1, -1),
        jnp.asarray(cos_table),
        jnp.asarray(sin_table),
        residual,
        output_weight,
        query_rotary.T,
        rotary_key.T,
        gate_weight,
        up_weight,
        down_weight,
    )


def solution(mesh):
    n_sp, n_tp = mesh.shape["sp"], mesh.shape["tp"]

    def program(*arrays):
        residual, gate_weight = arrays[0], arrays[11]
        fits = (
            n_tp == PAIR * PAIR
            and n_sp == PAIR**3
            and gate_weight.shape[0] * n_sp == residual.shape[1]
            and gate_weight.shape[0] % LANES == 0
            and gate_weight.shape[1] % LANES == 0
            and -(gate_weight.shape[1] // LANES) % (n_sp // PAIR) == 1
            and arrays[3].shape[0] == LANES
        )
        if fits:
            return fused(n_sp, *arrays)
        return on_device(*arrays)

    placed = (
        P(("sp", "tp"), None),
        P("sp", "tp"),
        P("sp", "tp"),
        P("sp", None),
        P("sp", None),
        P(),
        P(None, "tp"),
        P(None, "tp"),
        P("tp"),
        P("tp", None),
        P(),
        P("sp", "tp"),
        P("sp", "tp"),
        P("tp", "sp"),
    )
    return jax.shard_map(
        program, mesh=mesh, in_specs=placed, out_specs=P(("sp", "tp"), None), check_vma=False
    )
```
